32 devices in a mesh: rep: 2 (over x), fs: 8 (over z, y), tp: 2 (over core).
Axes of the slice: x: 2, y: 2, z: 4, core: 2. Of those that a mesh axis runs over, the one named last changes fastest.
Arguments:
- stream: bfloat16 [8192, 2048], P(('rep', 'fs'), 'tp'), may hold values from -6 to 6
- recurrent_norm_gain: float32 [2048], replicated, may hold values from 0.1 to 1.9
- feedforward_norm_gain: float32 [2048], replicated, may hold values from 0.1 to 1.9
- recurrent_input_weight: bfloat16 [2048, 2048], P('fs', 'tp'), may hold values from -0.125 to 0.125
- output_gate_weight: bfloat16 [2048, 2048], P('fs', 'tp'), may hold values from -0.125 to 0.125
- causal_filter_weight: bfloat16 [4, 2048], P(None, 'tp'), may hold values from -3 to 3
- decay_gate_matrix: bfloat16 [32, 64, 64], P('tp'), may hold values from -0.75 to 0.75
- input_gate_matrix: bfloat16 [32, 64, 64], P('tp'), may hold values from -0.75 to 0.75
- channel_decay_param: float32 [2048], P('tp'), may hold values from 3 to 10
- token_decay_offset: float32 [8192, 2048], P(('rep', 'fs'), 'tp'), may hold values from -0.7 to 0, as said below
- recurrent_output_weight: bfloat16 [2048, 2048], P('tp', 'fs'), may hold values from -0.125 to 0.125
- up_projection_weight: bfloat16 [2048, 6144], P('fs', 'tp'), may hold values from -0.125 to 0.125
- down_projection_weight: bfloat16 [6144, 2048], P('tp', 'fs'), may hold values from -0.078125 to 0.078125
Outputs:
- updated: bfloat16 [8192, 2048], P(('rep', 'fs'), 'tp')
The draws below stay inside these ranges and needn't reach their ends.
Inputs may be any that keep to these rules, and one draw needn't show every extreme that they name: `token_decay_offset`: zero except at a few positions, where a whole row is negative.
All inputs are finite; a program needn't handle non-finite values.
Results may differ from the reference program's by a relative error of at most 0.015.
Values may be sent and summed in bfloat16 or wider, within the bound.
A program may use at most 128 MiB of HBM per device.

```python
import jax
import jax.numpy as jnp
from jax import lax

D = 2048
FF = 6144
BLOCK = 64
CONV = 4
SEQ_LEN = 128
TOKENS = 8192
BLOCKS = 32
N_TP = 2


def draw_channel_decay_param(key, part):
    kind_key = jax.random.fold_in(key, 11)
    slow_key = jax.random.fold_in(key, 12)
    fast_key = jax.random.fold_in(key, 13)
    fast = jax.random.uniform(kind_key, (D,), jnp.float32) < 0.5
    slow_rate = jnp.exp(jax.random.uniform(slow_key, (D,), jnp.float32, jnp.log(0.3), jnp.log(3.0))) / SEQ_LEN
    fast_rate = jnp.exp(jax.random.uniform(fast_key, (D,), jnp.float32, jnp.log(0.1), jnp.log(0.3)))
    rate = jnp.where(fast, fast_rate, slow_rate)
    return (-jnp.log(jnp.expm1(rate / 8.0))).astype(jnp.float32)


def draw_token_decay_offset(key, part):
    where_key = jax.random.fold_in(key, 21)
    depth_key = jax.random.fold_in(key, 22)
    hits = jax.random.uniform(where_key, (TOKENS, 1), jnp.float32) < 3.0 / SEQ_LEN
    depth = jax.random.uniform(depth_key, (TOKENS, D), jnp.float32, 0.22, 0.69)
    return jnp.where(hits, -depth, 0.0).astype(jnp.float32)


def block_scale(own_key, shape, cuts, least, high):
    loudness = 1.0
    for position, blocks in cuts:
        heights = jax.random.uniform(jax.random.fold_in(jax.random.fold_in(own_key, 6), position), (blocks,), jnp.float32, least / len(cuts), high / len(cuts))
        loudness = loudness * jnp.repeat(jnp.exp(heights), shape[position] // blocks).reshape((-1,) + (1,) * (len(shape) - 1 - position))
    return loudness


def noise(rng, shape, width, most, shards=(), kind=jnp.bfloat16):
    array = width * jax.random.normal(rng, shape, jnp.float32)
    if shards:
        array = array * block_scale(rng, shape, shards, -0.22, 0.18)
    return jnp.clip(array, -most, most).astype(kind)


def setup_inputs(seed: int = 0) -> dict:
    seeds = jax.random.split(jax.random.key(seed), 14)
    return {
        "stream": noise(seeds[0], (TOKENS, D), 1.0, 6.0, ((0, 16), (1, 2))),
        "recurrent_norm_gain": jnp.clip(1.0 + 0.18 * jax.random.normal(seeds[1], (D,), jnp.float32), 0.1, 1.9),
        "feedforward_norm_gain": jnp.clip(1.0 + 0.18 * jax.random.normal(seeds[2], (D,), jnp.float32), 0.1, 1.9),
        "recurrent_input_weight": noise(seeds[3], (D, D), D ** -0.5, 0.125, ((0, 8), (1, 2))),
        "output_gate_weight": noise(seeds[4], (D, D), D ** -0.5, 0.125, ((0, 8), (1, 2))),
        "causal_filter_weight": noise(seeds[5], (CONV, D), CONV ** -0.5, 3.0, ((1, 2),)),
        "decay_gate_matrix": noise(seeds[6], (BLOCKS, BLOCK, BLOCK), BLOCK ** -0.5, 0.75, ((0, 2),)),
        "input_gate_matrix": noise(seeds[7], (BLOCKS, BLOCK, BLOCK), BLOCK ** -0.5, 0.75, ((0, 2),)),
        "channel_decay_param": draw_channel_decay_param(jax.random.fold_in(seeds[13], 71), 0),
        "token_decay_offset": draw_token_decay_offset(jax.random.fold_in(seeds[13], 71), 0),
        "recurrent_output_weight": noise(seeds[10], (D, D), D ** -0.5, 0.125, ((0, 2), (1, 8))),
        "up_projection_weight": noise(seeds[11], (D, FF), D ** -0.5, 0.125, ((0, 8), (1, 2))),
        "down_projection_weight": noise(seeds[12], (FF, D), FF ** -0.5, 0.078125, ((0, 2), (1, 8))),
    }


EPSILON = 1e-06
DECAY_MULTIPLIER = 8.0

def norm_rows(values, gain):
    widened = values.astype(jnp.float32)
    inverse = lax.rsqrt(lax.optimization_barrier(jnp.mean(widened * widened, axis=-1, keepdims=True)) + EPSILON)
    return (widened * inverse * gain).astype(jnp.bfloat16)

def short_filter(values, causal_filter_weight):
    positions, channels = values.shape
    sequences = positions // SEQ_LEN
    reach = causal_filter_weight.shape[0]
    widened = lax.optimization_barrier(values).astype(jnp.float32).reshape(sequences, SEQ_LEN, channels)
    padded = jnp.pad(widened, ((0, 0), (reach - 1, 0), (0, 0)))
    taps = causal_filter_weight.astype(jnp.float32)
    total = taps[0] * padded[:, 0:SEQ_LEN]
    for offset in range(1, reach):
        total = total + taps[offset] * padded[:, offset:offset + SEQ_LEN]
    return total.reshape(positions, channels).astype(jnp.bfloat16)

def combine(earlier, later):
    return (earlier[0] * later[0], later[0] * earlier[1] + later[1])

def recurrent_states(filtered_input, output_gate_rows, decay_gate_matrix, input_gate_matrix, channel_decay_param, token_decay_offset):
    positions, channels = filtered_input.shape
    blocks, block_size, _ = decay_gate_matrix.shape
    widened = lax.optimization_barrier(filtered_input).astype(jnp.float32)
    grouped = widened.reshape(positions, blocks, block_size)
    recurrent_step = jax.nn.sigmoid(jnp.einsum('tnc,ncd->tnd', grouped, decay_gate_matrix.astype(jnp.float32)).reshape(positions, channels))
    inputs = jax.nn.sigmoid(jnp.einsum('tnc,ncd->tnd', grouped, input_gate_matrix.astype(jnp.float32)).reshape(positions, channels))
    decay_logarithm = -DECAY_MULTIPLIER * recurrent_step * jax.nn.softplus(-channel_decay_param) + token_decay_offset
    drive = jnp.sqrt(-jnp.expm1(2.0 * decay_logarithm)) * inputs * widened
    shaped = (positions // SEQ_LEN, SEQ_LEN, channels)
    _, states = lax.associative_scan(combine, (jnp.exp(decay_logarithm).reshape(shaped), drive.reshape(shaped)), axis=1)
    gate_wide = lax.optimization_barrier(output_gate_rows).astype(jnp.float32)
    return (states.reshape(positions, channels) * jax.nn.gelu(gate_wide, approximate=False)).astype(jnp.bfloat16)

def reference(stream, recurrent_norm_gain, feedforward_norm_gain, recurrent_input_weight, output_gate_weight, causal_filter_weight, decay_gate_matrix, input_gate_matrix, channel_decay_param, token_decay_offset, recurrent_output_weight, up_projection_weight, down_projection_weight):
    normed = norm_rows(stream, recurrent_norm_gain)
    span = D // N_TP
    grouped_block_rows = span // BLOCK
    mixer_update = jnp.zeros(stream.shape, jnp.float32)
    for channel_group in range(N_TP):
        lower_bound = channel_group * span
        upper_bound = lower_bound + span
        values = jnp.dot(normed, recurrent_input_weight[:, lower_bound:upper_bound], preferred_element_type=jnp.float32).astype(jnp.bfloat16)
        gate_values = jnp.dot(normed, output_gate_weight[:, lower_bound:upper_bound], preferred_element_type=jnp.float32).astype(jnp.bfloat16)
        filtered_input = short_filter(values, causal_filter_weight[:, lower_bound:upper_bound])
        mixed_rows = recurrent_states(filtered_input, gate_values, decay_gate_matrix[channel_group * grouped_block_rows:(channel_group + 1) * grouped_block_rows], input_gate_matrix[channel_group * grouped_block_rows:(channel_group + 1) * grouped_block_rows], channel_decay_param[lower_bound:upper_bound], token_decay_offset[:, lower_bound:upper_bound])
        partial_value = jnp.dot(mixed_rows, recurrent_output_weight[lower_bound:upper_bound], preferred_element_type=jnp.float32).astype(jnp.bfloat16)
        mixer_update = mixer_update + lax.optimization_barrier(partial_value).astype(jnp.float32)
    middle = (stream.astype(jnp.float32) + mixer_update).astype(jnp.bfloat16)
    normed_mid = norm_rows(middle, feedforward_norm_gain)
    hidden_span = FF // N_TP
    channel_update = jnp.zeros(stream.shape, jnp.float32)
    for channel_group in range(N_TP):
        lower_bound = channel_group * hidden_span
        upper_bound = lower_bound + hidden_span
        raised = jnp.dot(normed_mid, up_projection_weight[:, lower_bound:upper_bound], preferred_element_type=jnp.float32)
        activity = jnp.square(jax.nn.relu(raised)).astype(jnp.bfloat16)
        partial_value = jnp.dot(activity, down_projection_weight[lower_bound:upper_bound], preferred_element_type=jnp.float32).astype(jnp.bfloat16)
        channel_update = channel_update + lax.optimization_barrier(partial_value).astype(jnp.float32)
    return (middle.astype(jnp.float32) + channel_update).astype(jnp.bfloat16)
```

```python
import functools

import jax
import jax.numpy as jnp
from jax import lax
from jax.experimental import pallas as pl
from jax.experimental.pallas import tpu as pltpu
from jax.sharding import PartitionSpec as P

SEQ_LEN = 128
EPSILON = 1e-06
DECAY_MULTIPLIER = 8.0
LANES = 128


def half(values, which, axis):
    first, second = jnp.split(values, 2, axis)
    return jnp.where(which == 0, first, second)


def gather_shard(shard, ids, sizes):
    rep, fs, _ = ids
    _, n_fs, _ = sizes
    own, for_peer = shard
    hops = n_fs // 2
    place, side = fs // 2, fs % 2
    from_peer = lax.ppermute(for_peer, "fs", [(i, i ^ 1) for i in range(n_fs)])
    own_first = side == rep
    mine = jnp.where(own_first, own, from_peer)
    whole = jnp.zeros((n_fs,) + own.shape, own.dtype)
    whole = put(whole, own, fs)
    whole = put(whole, from_peer, fs ^ 1)
    ring = [(i, (i + n_fs - 2) % n_fs) for i in range(n_fs)]
    for step in range(1, hops):
        mine = lax.ppermute(mine, "fs", ring)
        other = lax.ppermute(mine, "rep", [(0, 1), (1, 0)])
        base = 2 * ((place + step) % hops)
        whole = put(whole, mine, base + rep)
        whole = put(whole, other, base + 1 - rep)
    return whole


def put(whole, piece, index):
    return lax.dynamic_update_index_in_dim(whole, piece, index, 0)


def gather_features(values, tp, n_tp):
    if n_tp != 2:
        return lax.all_gather(values, "tp", axis=1, tiled=True)
    other = lax.ppermute(values, "tp", [(0, 1), (1, 0)])
    return jnp.where(
        tp == 0, jnp.concatenate([values, other], 1), jnp.concatenate([other, values], 1)
    )


def sum_features(parts, tp, n_tp):
    total = lax.dynamic_index_in_dim(parts, tp, 0, False).astype(jnp.float32)
    for shift in range(1, n_tp):
        piece = lax.dynamic_index_in_dim(parts, (tp + shift) % n_tp, 0, False)
        got = lax.ppermute(piece, "tp", [(i, (i + shift) % n_tp) for i in range(n_tp)])
        total = total + got.astype(jnp.float32)
    return total.astype(jnp.bfloat16)


def norm_rows(values, gain):
    widened = values.astype(jnp.float32)
    inverse = lax.rsqrt(jnp.mean(widened * widened, axis=-1, keepdims=True) + EPSILON)
    return (widened * inverse * gain).astype(jnp.bfloat16)


def columns_kernel(x_ref, w_ref, o_ref):
    o_ref[0] = jnp.dot(x_ref[...], w_ref[0], preferred_element_type=jnp.float32).astype(
        jnp.bfloat16
    )


def columns_matmul(x, weight, n_tp):
    tokens, depth = x.shape
    pieces, _, cols = weight.shape
    per = pieces // n_tp
    return pl.pallas_call(
        columns_kernel,
        grid=(pieces,),
        in_specs=[
            pl.BlockSpec((tokens, depth), lambda p: (0, 0)),
            pl.BlockSpec((1, depth, cols), lambda p: (p, 0, 0)),
        ],
        out_specs=pl.BlockSpec((1, tokens, cols), lambda p: (p // per, 0, p % per)),
        out_shape=jax.ShapeDtypeStruct((n_tp, tokens, per * cols), jnp.bfloat16),
        cost_estimate=pl.CostEstimate(
            flops=2 * tokens * depth * cols * pieces,
            bytes_accessed=2 * (tokens * depth + pieces * cols * (depth + tokens)),
            transcendentals=0,
        ),
        name="columns_matmul",
    )(x, weight)


def shift_down(values, rows, amount, fill):
    index = lax.broadcasted_iota(jnp.int32, values.shape, 0)
    return jnp.where(index < amount, fill, pltpu.roll(values, amount, 0))


def recurrence_kernel(value_ref, gate_ref, offset_ref, taps_ref, maps_ref, rate_ref, out_ref):
    rows, channels = value_ref.shape
    reach = taps_ref.shape[0]
    for tile in range(channels // LANES):
        cols = slice(tile * LANES, (tile + 1) * LANES)
        values = value_ref[:, cols].astype(jnp.float32)
        filtered = taps_ref[reach - 1 : reach, cols] * values
        for back in range(1, reach):
            tap = taps_ref[reach - 1 - back : reach - back, cols]
            filtered = filtered + tap * shift_down(values, rows, back, 0.0)
        conved = filtered.astype(jnp.bfloat16)
        logits = jnp.dot(conved, maps_ref[tile], preferred_element_type=jnp.float32)
        steps = 1.0 / (1.0 + jnp.exp(-logits))
        log_decay = steps[:, :LANES] * rate_ref[:, cols] + offset_ref[:, cols]
        decay = jnp.exp(log_decay)
        y = -2.0 * log_decay
        series = 1.0 + y * (
            -1 / 2 + y * (1 / 6 + y * (-1 / 24 + y * (1 / 120 + y * (-1 / 720 + y * (1 / 5040)))))
        )
        lost = jnp.where(y < 0.35, y * series, 1.0 - decay * decay)
        state = jnp.sqrt(lost) * steps[:, LANES:] * conved.astype(jnp.float32)
        span = 1
        while span < rows:
            state = state + decay * shift_down(state, rows, span, 0.0)
            if span * 2 < rows:
                decay = decay * shift_down(decay, rows, span, 1.0)
            span *= 2
        gate = gate_ref[:, cols].astype(jnp.float32)
        gelu = 0.5 * gate * (1.0 + lax.erf(gate * 0.7071067811865476))
        out_ref[:, cols] = (state * gelu).astype(jnp.bfloat16)


def recurrence(projected, offset, taps, decay_maps, input_maps, rate):
    tokens, channels = offset.shape
    blocks, size, _ = decay_maps.shape
    per = LANES // size

    def diagonal(maps):
        grouped = maps.reshape(blocks // per, per, size, size)
        eye = jnp.eye(per, dtype=maps.dtype)
        spread = grouped[:, :, :, None, :] * eye[None, :, None, :, None]
        return spread.reshape(blocks // per, LANES, LANES)

    maps = jnp.concatenate([diagonal(decay_maps), diagonal(input_maps)], 2)
    return pl.pallas_call(
        recurrence_kernel,
        grid=(tokens // SEQ_LEN,),
        in_specs=[
            pl.BlockSpec((SEQ_LEN, channels), lambda s: (s, 0)),
            pl.BlockSpec((SEQ_LEN, channels), lambda s: (s, 1)),
            pl.BlockSpec((SEQ_LEN, channels), lambda s: (s, 0)),
            pl.BlockSpec(taps.shape, lambda s: (0, 0)),
            pl.BlockSpec(maps.shape, lambda s: (0, 0, 0)),
            pl.BlockSpec((1, channels), lambda s: (0, 0)),
        ],
        out_specs=pl.BlockSpec((SEQ_LEN, channels), lambda s: (s, 0)),
        out_shape=jax.ShapeDtypeStruct((tokens, channels), jnp.bfloat16),
        cost_estimate=pl.CostEstimate(
            flops=tokens * channels * 700,
            bytes_accessed=tokens * channels * 10,
            transcendentals=tokens * channels * 6,
        ),
        name="recurrence",
    )(projected, projected, offset, taps.astype(jnp.float32), maps, rate[None, :])


def shards(
    sizes,
    stream,
    recurrent_norm_gain,
    feedforward_norm_gain,
    recurrent_input_weight,
    output_gate_weight,
    causal_filter_weight,
    decay_gate_matrix,
    input_gate_matrix,
    channel_decay_param,
    token_decay_offset,
    recurrent_output_weight,
    up_projection_weight,
    down_projection_weight,
):
    n_rep, n_fs, n_tp = sizes
    ids = lax.axis_index("rep"), lax.axis_index("fs"), lax.axis_index("tp")
    _, fs, tp = ids
    side = fs % 2
    pairs = [(i, i ^ 1) for i in range(n_fs)]
    tokens = stream.shape[0]

    def halves(weight, axis):
        return half(weight, side, axis), half(weight, 1 - side, axis)

    def to_peer(values):
        return lax.ppermute(values, "fs", pairs)

    value_own, value_peer = halves(recurrent_input_weight, 1)
    gate_own, gate_peer = halves(output_gate_weight, 1)
    entry = (
        jnp.concatenate([value_own, gate_own], 1),
        jnp.concatenate([value_peer, gate_peer], 1),
    )
    entry_full = gather_shard(entry, ids, sizes)
    stream_peer = to_peer(stream)
    offset_own, offset_send = halves(token_decay_offset, 1)
    offset_peer = to_peer(offset_send.astype(jnp.bfloat16)).astype(jnp.float32)
    output_full = gather_shard(halves(recurrent_output_weight, 0), ids, sizes)
    expand_full = gather_shard(halves(up_projection_weight, 1), ids, sizes)
    contract_full = gather_shard(halves(down_projection_weight, 0), ids, sizes)

    own_pair = jnp.concatenate([stream, stream_peer], 0)
    whole = gather_features(own_pair, tp, n_tp)
    normed = norm_rows(whole, recurrent_norm_gain)
    width = whole.shape[1]
    projected = jnp.dot(
        normed, entry_full.reshape(width, -1), preferred_element_type=jnp.float32
    ).astype(jnp.bfloat16)
    mixed = recurrence(
        projected,
        jnp.concatenate([offset_own, offset_peer], 0),
        half(causal_filter_weight, side, 1),
        half(decay_gate_matrix, side, 0),
        half(input_gate_matrix, side, 0),
        half(-DECAY_MULTIPLIER * jax.nn.softplus(-channel_decay_param), side, 0),
    )
    mixer_chip = sum_features(columns_matmul(mixed, output_full, n_tp), tp, n_tp)
    got_own = to_peer(mixer_chip[tokens:])
    got_peer = to_peer(mixer_chip[:tokens])
    update = mixer_chip.astype(jnp.float32) + jnp.concatenate([got_own, got_peer], 0).astype(
        jnp.float32
    )
    middle = (own_pair.astype(jnp.float32) + update).astype(jnp.bfloat16)
    normed_mid = norm_rows(gather_features(middle, tp, n_tp), feedforward_norm_gain)
    raised = jnp.dot(
        normed_mid, expand_full.reshape(width, -1), preferred_element_type=jnp.float32
    )
    activity = jnp.square(jax.nn.relu(raised)).astype(jnp.bfloat16)
    peer_chip = sum_features(columns_matmul(activity[tokens:], contract_full, n_tp), tp, n_tp)
    got = to_peer(peer_chip)
    own_chip = sum_features(columns_matmul(activity[:tokens], contract_full, n_tp), tp, n_tp)
    channel_sum = own_chip.astype(jnp.float32) + got.astype(jnp.float32)
    return (middle[:tokens].astype(jnp.float32) + channel_sum).astype(jnp.bfloat16)


def solution(mesh):
    in_specs = (
        P(("rep", "fs"), "tp"),
        P(),
        P(),
        P("fs", "tp"),
        P("fs", "tp"),
        P(None, "tp"),
        P("tp", None, None),
        P("tp", None, None),
        P("tp"),
        P(("rep", "fs"), "tp"),
        P("tp", "fs"),
        P("fs", "tp"),
        P("tp", "fs"),
    )
    out_specs = P(("rep", "fs"), "tp")
    sizes = tuple(mesh.shape[axis] for axis in ("rep", "fs", "tp"))
    return jax.shard_map(
        functools.partial(shards, sizes),
        mesh=mesh,
        in_specs=in_specs,
        out_specs=out_specs,
        check_vma=False,
    )
```

```python
import jax
import jax.numpy as jnp
from jax import lax
from jax.experimental import pallas as pl
from jax.experimental.pallas import tpu as pltpu
from jax.sharding import PartitionSpec as P


SEQ_LEN = 128
EPSILON = 1e-06
DECAY_MULTIPLIER = 8.0
LANES = 128


def half(values, which, axis):
    first, second = jnp.split(values, 2, axis)
    return jnp.where(which == 0, first, second)


def gather_shard(shard, ids, sizes):
    rep, fs, _ = ids
    _, n_fs, _ = sizes
    own, for_peer = shard
    hops = n_fs // 2
    place, side = fs // 2, fs % 2
    from_peer = lax.ppermute(for_peer, "fs", [(i, i ^ 1) for i in range(n_fs)])
    own_first = side == rep
    mine = jnp.where(own_first, own, from_peer)
    whole = jnp.zeros((n_fs,) + own.shape, own.dtype)
    whole = put(whole, own, fs)
    whole = put(whole, from_peer, fs ^ 1)
    ring = [(i, (i + n_fs - 2) % n_fs) for i in range(n_fs)]
    for step in range(1, hops):
        mine = lax.ppermute(mine, "fs", ring)
        other = lax.ppermute(mine, "rep", [(0, 1), (1, 0)])
        base = 2 * ((place + step) % hops)
        whole = put(whole, mine, base + rep)
        whole = put(whole, other, base + 1 - rep)
    return whole


def put(whole, piece, index):
    return lax.dynamic_update_index_in_dim(whole, piece, index, 0)


def gather_features(values, tp, n_tp):
    if n_tp != 2:
        return lax.all_gather(values, "tp", axis=1, tiled=True)
    other = lax.ppermute(values, "tp", [(0, 1), (1, 0)])
    return jnp.where(
        tp == 0, jnp.concatenate([values, other], 1), jnp.concatenate([other, values], 1)
    )


def sum_features(parts, tp, n_tp):
    total = lax.dynamic_index_in_dim(parts, tp, 0, False).astype(jnp.float32)
    for shift in range(1, n_tp):
        piece = lax.dynamic_index_in_dim(parts, (tp + shift) % n_tp, 0, False)
        got = lax.ppermute(piece, "tp", [(i, (i + shift) % n_tp) for i in range(n_tp)])
        total = total + got.astype(jnp.float32)
    return total.astype(jnp.bfloat16)


def norm_rows(values, gain):
    widened = values.astype(jnp.float32)
    inverse = lax.rsqrt(jnp.mean(widened * widened, axis=-1, keepdims=True) + EPSILON)
    return (widened * inverse * gain).astype(jnp.bfloat16)


def columns_kernel(x_ref, w_ref, o_ref):
    o_ref[0] = jnp.dot(x_ref[...], w_ref[0], preferred_element_type=jnp.float32).astype(
        jnp.bfloat16
    )


def columns_matmul(x, weight, n_tp):
    tokens, depth = x.shape
    pieces, _, cols = weight.shape
    per = pieces // n_tp
    return pl.pallas_call(
        columns_kernel,
        grid=(pieces,),
        in_specs=[
            pl.BlockSpec((tokens, depth), lambda p: (0, 0)),
            pl.BlockSpec((1, depth, cols), lambda p: (p, 0, 0)),
        ],
        out_specs=pl.BlockSpec((1, tokens, cols), lambda p: (p // per, 0, p % per)),
        out_shape=jax.ShapeDtypeStruct((n_tp, tokens, per * cols), jnp.bfloat16),
        cost_estimate=pl.CostEstimate(
            flops=2 * tokens * depth * cols * pieces,
            bytes_accessed=2 * (tokens * depth + pieces * cols * (depth + tokens)),
            transcendentals=0,
        ),
        name="columns_matmul",
    )(x, weight)


def shift_down(values, amount, fill):
    index = lax.broadcasted_iota(jnp.int32, values.shape, 0)
    return jnp.where(index < amount, fill, pltpu.roll(values, amount, 0))


def recurrence_kernel(value_ref, gate_ref, offset_ref, taps_ref, maps_ref, rate_ref, out_ref):
    rows, channels = value_ref.shape
    reach = taps_ref.shape[0]
    for tile in range(channels // LANES):
        cols = slice(tile * LANES, (tile + 1) * LANES)
        values = value_ref[:, cols].astype(jnp.float32)
        filtered = taps_ref[reach - 1 : reach, cols] * values
        for back in range(1, reach):
            tap = taps_ref[reach - 1 - back : reach - back, cols]
            filtered = filtered + tap * shift_down(values, back, 0.0)
        conved = filtered.astype(jnp.bfloat16)
        logits = jnp.dot(conved, maps_ref[tile], preferred_element_type=jnp.float32)
        steps = 1.0 / (1.0 + jnp.exp(-logits))
        log_decay = steps[:, :LANES] * rate_ref[:, cols] + offset_ref[:, cols]
        decay = jnp.exp(log_decay)
        y = -2.0 * log_decay
        series = 1.0 + y * (
            -1 / 2 + y * (1 / 6 + y * (-1 / 24 + y * (1 / 120 + y * (-1 / 720 + y * (1 / 5040)))))
        )
        lost = jnp.where(y < 0.35, y * series, 1.0 - decay * decay)
        state = jnp.sqrt(lost) * steps[:, LANES:] * conved.astype(jnp.float32)
        span = 1
        while span < rows:
            state = state + decay * shift_down(state, span, 0.0)
            if span * 2 < rows:
                decay = decay * shift_down(decay, span, 1.0)
            span *= 2
        gate = gate_ref[:, cols].astype(jnp.float32)
        gelu = 0.5 * gate * (1.0 + lax.erf(gate * 0.7071067811865476))
        out_ref[:, cols] = (state * gelu).astype(jnp.bfloat16)


def recurrence(projected, offset, taps, decay_maps, input_maps, rate):
    tokens, channels = offset.shape
    blocks, size, _ = decay_maps.shape
    per = LANES // size

    def diagonal(maps):
        grouped = maps.reshape(blocks // per, per, size, size)
        eye = jnp.eye(per, dtype=maps.dtype)
        spread = grouped[:, :, :, None, :] * eye[None, :, None, :, None]
        return spread.reshape(blocks // per, LANES, LANES)

    maps = jnp.concatenate([diagonal(decay_maps), diagonal(input_maps)], 2)
    return pl.pallas_call(
        recurrence_kernel,
        grid=(tokens // SEQ_LEN,),
        in_specs=[
            pl.BlockSpec((SEQ_LEN, channels), lambda s: (s, 0)),
            pl.BlockSpec((SEQ_LEN, channels), lambda s: (s, 1)),
            pl.BlockSpec((SEQ_LEN, channels), lambda s: (s, 0)),
            pl.BlockSpec(taps.shape, lambda s: (0, 0)),
            pl.BlockSpec(maps.shape, lambda s: (0, 0, 0)),
            pl.BlockSpec((1, channels), lambda s: (0, 0)),
        ],
        out_specs=pl.BlockSpec((SEQ_LEN, channels), lambda s: (s, 0)),
        out_shape=jax.ShapeDtypeStruct((tokens, channels), jnp.bfloat16),
        cost_estimate=pl.CostEstimate(
            flops=tokens * channels * 700,
            bytes_accessed=tokens * channels * 10,
            transcendentals=tokens * channels * 6,
        ),
        name="recurrence",
    )(projected, projected, offset, taps.astype(jnp.float32), maps, rate[None, :])


def shards(
    sizes,
    stream,
    recurrent_norm_gain,
    feedforward_norm_gain,
    recurrent_input_weight,
    output_gate_weight,
    causal_filter_weight,
    decay_gate_matrix,
    input_gate_matrix,
    channel_decay_param,
    token_decay_offset,
    recurrent_output_weight,
    up_projection_weight,
    down_projection_weight,
):
    _, n_fs, n_tp = sizes
    ids = lax.axis_index("rep"), lax.axis_index("fs"), lax.axis_index("tp")
    _, fs, tp = ids
    side = fs % 2
    pairs = [(i, i ^ 1) for i in range(n_fs)]
    tokens = stream.shape[0]

    def halves(weight, axis):
        return half(weight, side, axis), half(weight, 1 - side, axis)

    def to_peer(values):
        return lax.ppermute(values, "fs", pairs)

    value_own, value_peer = halves(recurrent_input_weight, 1)
    gate_own, gate_peer = halves(output_gate_weight, 1)
    entry = (
        jnp.concatenate([value_own, gate_own], 1),
        jnp.concatenate([value_peer, gate_peer], 1),
    )
    entry_full = gather_shard(entry, ids, sizes)
    stream_peer = to_peer(stream)
    offset_own, offset_send = halves(token_decay_offset, 1)
    offset_peer = to_peer(offset_send.astype(jnp.bfloat16)).astype(jnp.float32)
    output_full = gather_shard(halves(recurrent_output_weight, 0), ids, sizes)
    expand_full = gather_shard(halves(up_projection_weight, 1), ids, sizes)
    contract_full = gather_shard(halves(down_projection_weight, 0), ids, sizes)

    own_pair = jnp.concatenate([stream, stream_peer], 0)
    whole = gather_features(own_pair, tp, n_tp)
    normed = norm_rows(whole, recurrent_norm_gain)
    width = whole.shape[1]
    projected = jnp.dot(
        normed, entry_full.reshape(width, -1), preferred_element_type=jnp.float32
    ).astype(jnp.bfloat16)
    mixed = recurrence(
      projected,
      jnp.concatenate([offset_own, offset_peer], 0),
      half(causal_filter_weight, side, 1),
      half(decay_gate_matrix, side, 0),
      half(input_gate_matrix, side, 0),
      half(-DECAY_MULTIPLIER * jax.nn.softplus(-channel_decay_param), side, 0),
    )
    mixer_terms = columns_matmul(mixed, output_full, n_tp)
    mixer_chip = sum_features(mixer_terms, tp, n_tp)
    got_own = to_peer(mixer_chip[tokens:])
    got_peer = to_peer(mixer_chip[:tokens])
    update = mixer_chip.astype(jnp.float32) + jnp.concatenate([got_own, got_peer], 0).astype(
        jnp.float32
    )
    middle = (own_pair.astype(jnp.float32) + update).astype(jnp.bfloat16)
    normed_mid = norm_rows(gather_features(middle, tp, n_tp), feedforward_norm_gain)
    raised = jnp.dot(
        normed_mid, expand_full.reshape(width, -1), preferred_element_type=jnp.float32
    )
    activity = jnp.square(jax.nn.relu(raised)).astype(jnp.bfloat16)
    peer_chip = sum_features(columns_matmul(activity[tokens:], contract_full, n_tp), tp, n_tp)
    got = to_peer(peer_chip)
    own_chip = sum_features(columns_matmul(activity[:tokens], contract_full, n_tp), tp, n_tp)
    channel_sum = own_chip.astype(jnp.float32) + got.astype(jnp.float32)
    return (middle[:tokens].astype(jnp.float32) + channel_sum).astype(jnp.bfloat16)


def solution(mesh):
    in_specs = (
        P(("rep", "fs"), "tp"),
        P(),
        P(),
        P("fs", "tp"),
        P("fs", "tp"),
        P(None, "tp"),
        P("tp", None, None),
        P("tp", None, None),
        P("tp"),
        P(("rep", "fs"), "tp"),
        P("tp", "fs"),
        P("fs", "tp"),
        P("tp", "fs"),
    )
    out_specs = P(("rep", "fs"), "tp")
    sizes = tuple(mesh.shape[axis] for axis in ("rep", "fs", "tp"))

    def body(*args):
        return shards(sizes, *args)

    return jax.shard_map(
        body, mesh=mesh, in_specs=in_specs, out_specs=out_specs, check_vma=False
    )
```

```python
import functools

import jax
import jax.numpy as jnp
from jax import lax
from jax.experimental import pallas as pl
from jax.experimental.pallas import tpu as pltpu
from jax.sharding import PartitionSpec as P


SEQ_LEN = 128
EPSILON = 1e-06
DECAY_MULTIPLIER = 8.0
LANES = 128


def half(values, which, axis):
    first, second = jnp.split(values, 2, axis)
    return jnp.where(which == 0, first, second)


def gather_shard(shard, ids, sizes):
    rep, fs, _ = ids
    _, n_fs, _ = sizes
    own, for_peer = shard
    hops = n_fs // 2
    place, side = fs // 2, fs % 2
    from_peer = lax.ppermute(for_peer, "fs", [(i, i ^ 1) for i in range(n_fs)])
    start = jnp.where(side == rep, own, from_peer)
    up = [(i, (i + 2) % n_fs) for i in range(n_fs)]
    down = [(i, (i + n_fs - 2) % n_fs) for i in range(n_fs)]
    pieces, places = [own, from_peer], [fs, fs ^ 1]
    below = above = start
    for step in range(1, hops):
        if step % 2:
            below = mine = lax.ppermute(below, "fs", up)
            base = 2 * ((place + hops - (step + 1) // 2) % hops)
        else:
            above = mine = lax.ppermute(above, "fs", down)
            base = 2 * ((place + step // 2) % hops)
        pieces += [mine, lax.ppermute(mine, "rep", [(0, 1), (1, 0)])]
        places += [base + rep, base + 1 - rep]
    return pieces, jnp.stack(places).astype(jnp.int32)


def gather_features(values, tp, n_tp):
    if n_tp != 2:
        return lax.all_gather(values, "tp", axis=1, tiled=True)
    other = lax.ppermute(values, "tp", [(0, 1), (1, 0)])
    return jnp.where(
        tp == 0, jnp.concatenate([values, other], 1), jnp.concatenate([other, values], 1)
    )


def sum_features(parts, tp, n_tp):
    total = lax.dynamic_index_in_dim(parts, tp, 0, False).astype(jnp.float32)
    for shift in range(1, n_tp):
        piece = lax.dynamic_index_in_dim(parts, (tp + shift) % n_tp, 0, False)
        got = lax.ppermute(piece, "tp", [(i, (i + shift) % n_tp) for i in range(n_tp)])
        total = total + got.astype(jnp.float32)
    return total.astype(jnp.bfloat16)


def norm_rows(values, gain):
    widened = values.astype(jnp.float32)
    inverse = lax.rsqrt(jnp.mean(widened * widened, axis=-1, keepdims=True) + EPSILON)
    return (widened * inverse * gain).astype(jnp.bfloat16)


ROWS = 256
CHUNK = 512


def depth_kernel(squared, places_ref, x_ref, *refs):
    *pieces, out_ref = refs
    depth, width = pieces[0].shape
    chunk = min(CHUNK, width)
    for lower in range(0, width, chunk):
        cols = slice(lower, lower + chunk)
        total = None
        for index, piece in enumerate(pieces):
            place = pl.multiple_of(places_ref[index] * depth, depth)
            term = jnp.dot(
                x_ref[:, pl.ds(place, depth)], piece[:, cols], preferred_element_type=jnp.float32
            )
            total = term if total is None else total + term
        if squared:
            total = jnp.square(jnp.maximum(total, 0.0))
        out_ref[:, cols] = total.astype(jnp.bfloat16)


def depth_matmul(x, gathered, squared=False):
    pieces, places = gathered
    tokens, width = x.shape
    shape = pieces[0].shape
    return pl.pallas_call(
        functools.partial(depth_kernel, squared),
        grid_spec=pltpu.PrefetchScalarGridSpec(
            num_scalar_prefetch=1,
            grid=(tokens // ROWS,),
            in_specs=[pl.BlockSpec((ROWS, width), lambda m, _: (m, 0))]
            + [pl.BlockSpec(shape, lambda m, _: (0, 0))] * len(pieces),
            out_specs=pl.BlockSpec((ROWS, shape[1]), lambda m, _: (m, 0)),
        ),
        out_shape=jax.ShapeDtypeStruct((tokens, shape[1]), jnp.bfloat16),
        cost_estimate=pl.CostEstimate(
            flops=2 * tokens * width * shape[1],
            bytes_accessed=2 * (tokens * width + (tokens + width) * shape[1]),
            transcendentals=0,
        ),
        name="depth_matmul",
    )(places, x, *pieces)


def columns_kernel(per, places_ref, x_ref, *refs):
    *pieces, out_ref = refs
    cols = pieces[0].shape[1]
    for index, piece in enumerate(pieces):
        place = places_ref[index]
        lower = pl.multiple_of((place % per) * cols, cols)
        out_ref[place // per, :, pl.ds(lower, cols)] = jnp.dot(
            x_ref[...], piece[...], preferred_element_type=jnp.float32
        ).astype(jnp.bfloat16)


def columns_matmul(x, gathered, n_tp, first, tokens):
    pieces, places = gathered
    depth, cols = pieces[0].shape
    per = len(pieces) // n_tp
    skip = first // ROWS
    return pl.pallas_call(
        functools.partial(columns_kernel, per),
        grid_spec=pltpu.PrefetchScalarGridSpec(
            num_scalar_prefetch=1,
            grid=(tokens // ROWS,),
            in_specs=[pl.BlockSpec((ROWS, depth), lambda m, _: (m + skip, 0))]
            + [pl.BlockSpec((depth, cols), lambda m, _: (0, 0))] * len(pieces),
            out_specs=pl.BlockSpec((n_tp, ROWS, per * cols), lambda m, _: (0, m, 0)),
        ),
        out_shape=jax.ShapeDtypeStruct((n_tp, tokens, per * cols), jnp.bfloat16),
        cost_estimate=pl.CostEstimate(
            flops=2 * tokens * depth * cols * len(pieces),
            bytes_accessed=2 * (tokens * depth + len(pieces) * cols * (depth + tokens)),
            transcendentals=0,
        ),
        name="columns_matmul",
    )(places, x, *pieces)


def shift_down(values, amount, fill):
    index = lax.broadcasted_iota(jnp.int32, values.shape, 0)
    return jnp.where(index < amount, fill, pltpu.roll(values, amount, 0))


def recurrence_kernel(
    side_ref, value_ref, gate_ref, own_ref, peer_ref, taps_ref, maps_ref, rate_ref, out_ref
):
    rows, channels = value_ref.shape
    reach = taps_ref.shape[0]
    per = LANES // maps_ref.shape[1]
    is_own = pl.program_id(0) < pl.num_programs(0) // 2
    for tile in range(channels // LANES):
        cols = slice(tile * LANES, (tile + 1) * LANES)
        values = value_ref[:, cols].astype(jnp.float32)
        filtered = taps_ref[reach - 1 : reach, cols] * values
        for back in range(1, reach):
            tap = taps_ref[reach - 1 - back : reach - back, cols]
            filtered = filtered + tap * shift_down(values, back, 0.0)
        conved = filtered.astype(jnp.bfloat16)
        maps = maps_ref[tile * per : (tile + 1) * per].reshape(LANES, 2 * LANES)
        logits = jnp.dot(conved, maps, preferred_element_type=jnp.float32)
        offset = jnp.where(is_own, own_ref[:, cols], peer_ref[:, cols].astype(jnp.float32))
        steps = 1.0 / (1.0 + jnp.exp(-logits))
        log_decay = steps[:, :LANES] * rate_ref[:, cols] + offset
        decay = jnp.exp(log_decay)
        y = -2.0 * log_decay
        series = 1.0 + y * (
            -1 / 2 + y * (1 / 6 + y * (-1 / 24 + y * (1 / 120 + y * (-1 / 720 + y * (1 / 5040)))))
        )
        lost = jnp.where(y < 0.35, y * series, 1.0 - decay * decay)
        state = jnp.sqrt(lost) * steps[:, LANES:] * conved.astype(jnp.float32)
        span = 1
        while span < rows:
            state = state + decay * shift_down(state, span, 0.0)
            if span * 2 < rows:
                decay = decay * shift_down(decay, span, 1.0)
            span *= 2
        gate = gate_ref[:, cols].astype(jnp.float32)
        gelu = 0.5 * gate * (1.0 + lax.erf(gate * 0.7071067811865476))
        out_ref[:, cols] = (state * gelu).astype(jnp.bfloat16)


def recurrence(projected, offset_own, offset_peer, taps, decay_maps, input_maps, rate, side):
    tokens = projected.shape[0]
    channels = offset_peer.shape[1]
    blocks, size, _ = decay_maps.shape
    per = LANES // size
    block = jnp.arange(blocks)[:, None, None] % per
    group = jnp.arange(LANES)[None, None, :] // size

    def diagonal(maps):
        return jnp.where(block == group, jnp.tile(maps, (1, 1, per)), 0)

    maps = jnp.concatenate([diagonal(decay_maps), diagonal(input_maps)], 2)
    sequences = tokens // SEQ_LEN
    own = sequences // 2
    return pl.pallas_call(
        recurrence_kernel,
        grid_spec=pltpu.PrefetchScalarGridSpec(
            num_scalar_prefetch=1,
            grid=(sequences,),
            in_specs=[
                pl.BlockSpec((SEQ_LEN, channels), lambda s, side: (s, 0)),
                pl.BlockSpec((SEQ_LEN, channels), lambda s, side: (s, 1)),
                pl.BlockSpec(
                    (SEQ_LEN, channels), lambda s, side: (jnp.minimum(s, own - 1), side[0])
                ),
                pl.BlockSpec((SEQ_LEN, channels), lambda s, side: (jnp.maximum(s - own, 0), 0)),
                pl.BlockSpec((taps.shape[0], channels), lambda s, side: (0, side[0])),
                pl.BlockSpec((blocks // 2, size, 2 * LANES), lambda s, side: (side[0], 0, 0)),
                pl.BlockSpec((1, channels), lambda s, side: (0, side[0])),
            ],
            out_specs=pl.BlockSpec((SEQ_LEN, channels), lambda s, side: (s, 0)),
        ),
        out_shape=jax.ShapeDtypeStruct((tokens, channels), jnp.bfloat16),
        cost_estimate=pl.CostEstimate(
            flops=tokens * channels * 700,
            bytes_accessed=tokens * channels * 10,
            transcendentals=tokens * channels * 6,
        ),
        name="recurrence",
    )(
        side.astype(jnp.int32)[None],
        projected,
        projected,
        offset_own,
        offset_peer,
        taps.astype(jnp.float32),
        maps,
        rate[None, :],
    )


def shards(
    sizes,
    stream,
    recurrent_norm_gain,
    feedforward_norm_gain,
    recurrent_input_weight,
    output_gate_weight,
    causal_filter_weight,
    decay_gate_matrix,
    input_gate_matrix,
    channel_decay_param,
    token_decay_offset,
    recurrent_output_weight,
    up_projection_weight,
    down_projection_weight,
):
    _, n_fs, n_tp = sizes
    ids = lax.axis_index("rep"), lax.axis_index("fs"), lax.axis_index("tp")
    _, fs, tp = ids
    side = fs % 2
    pairs = [(i, i ^ 1) for i in range(n_fs)]
    tokens = stream.shape[0]

    def halves(weight, axis):
        return half(weight, side, axis), half(weight, 1 - side, axis)

    def to_peer(values):
        return lax.ppermute(values, "fs", pairs)

    value_own, value_peer = halves(recurrent_input_weight, 1)
    gate_own, gate_peer = halves(output_gate_weight, 1)
    entry = (
        jnp.concatenate([value_own, gate_own], 1),
        jnp.concatenate([value_peer, gate_peer], 1),
    )
    entry_full = gather_shard(entry, ids, sizes)
    stream_peer = to_peer(stream)
    offset_peer = to_peer(half(token_decay_offset, 1 - side, 1).astype(jnp.bfloat16))
    output_full = gather_shard(halves(recurrent_output_weight, 0), ids, sizes)
    expand_full = gather_shard(halves(up_projection_weight, 1), ids, sizes)
    contract_full = gather_shard(halves(down_projection_weight, 0), ids, sizes)

    own_pair = jnp.concatenate([stream, stream_peer], 0)
    whole = gather_features(own_pair, tp, n_tp)
    normed = norm_rows(whole, recurrent_norm_gain)
    projected = depth_matmul(normed, entry_full)
    mixed = recurrence(
        projected,
        token_decay_offset,
        offset_peer,
        causal_filter_weight,
        decay_gate_matrix,
        input_gate_matrix,
        -DECAY_MULTIPLIER * jax.nn.softplus(-channel_decay_param),
        side,
    )
    mixer_terms = columns_matmul(mixed, output_full, n_tp, 0, 2 * tokens)
    mixer_chip = sum_features(mixer_terms, tp, n_tp)
    got_own = to_peer(mixer_chip[tokens:])
    got_peer = to_peer(mixer_chip[:tokens])
    update = mixer_chip.astype(jnp.float32) + jnp.concatenate([got_own, got_peer], 0).astype(
        jnp.float32
    )
    middle = (own_pair.astype(jnp.float32) + update).astype(jnp.bfloat16)
    normed_mid = norm_rows(gather_features(middle, tp, n_tp), feedforward_norm_gain)
    activity = depth_matmul(normed_mid, expand_full, squared=True)
    peer_terms = columns_matmul(activity, contract_full, n_tp, tokens, tokens)
    got = to_peer(sum_features(peer_terms, tp, n_tp))
    own_terms = columns_matmul(activity, contract_full, n_tp, 0, tokens)
    own_chip = sum_features(own_terms, tp, n_tp)
    channel_sum = own_chip.astype(jnp.float32) + got.astype(jnp.float32)
    return (middle[:tokens].astype(jnp.float32) + channel_sum).astype(jnp.bfloat16)


def solution(mesh):
    in_specs = (
        P(("rep", "fs"), "tp"),
        P(),
        P(),
        P("fs", "tp"),
        P("fs", "tp"),
        P(None, "tp"),
        P("tp", None, None),
        P("tp", None, None),
        P("tp"),
        P(("rep", "fs"), "tp"),
        P("tp", "fs"),
        P("fs", "tp"),
        P("tp", "fs"),
    )
    out_specs = P(("rep", "fs"), "tp")
    sizes = tuple(mesh.shape[axis] for axis in ("rep", "fs", "tp"))

    def body(*args):
        return shards(sizes, *args)

    return jax.shard_map(
        body, mesh=mesh, in_specs=in_specs, out_specs=out_specs, check_vma=False
    )
```
